32 devices in a mesh: sp: 8 (over z, x), tp: 4 (over y, core).
Axes of the slice: x: 2, y: 2, z: 4, core: 2. Of those that a mesh axis runs over, the one named last changes fastest.
Arguments:
- block_input: bfloat16 [16384, 4096], P('sp'), may hold values from -6 to 6
- value_weight: bfloat16 [4096, 1024], P(None, 'tp'), may hold values from -0.09375 to 0.09375
- key_rows: bfloat16 [16384, 512], P('sp', 'tp'), may hold values from -1 to 1
- query_rows: bfloat16 [16384, 512], P('sp', 'tp'), may hold values from -1 to 1
- decay_pre: float32 [16, 16384], P('tp', 'sp'), may hold values from -3 to 2
- decay_log: float32 [16], P('tp'), may hold values from -16 to -2
- gate_rows: bfloat16 [16384, 1024], P('sp', 'tp'), may hold values from -6 to 6
- out_grad: bfloat16 [16384, 1024], P('sp', 'tp'), may hold values from -6 to 6
Outputs:
- key_grad: float32 [16384, 512], P('sp', 'tp')
- query_grad: float32 [16384, 512], P('sp', 'tp')
- decay_grad: float32 [16, 16384], P('tp', 'sp')
- gate_grad: float32 [16384, 1024], P('sp', 'tp')
- weight_grad: float32 [4096, 1024], P('sp', 'tp')
- row_norms: float32 [4096], P('sp')
The draws below stay inside these ranges and needn't reach their ends.
All inputs are finite; a program needn't handle non-finite values.
Results may differ from the reference program's by a relative error of at most 0.0035.
Values sent between devices are 32-bit elements; how exact they have to be, the bound alone decides.
A program may use at most 128 MiB of HBM per device.

```python
import jax
import jax.numpy as jnp
from jax import lax

D = 4096
HEADS = 16
HEAD = 64
GROUPS = 8
STATE = 64
BLK = 128
TOK_DEV = 2048
TOKENS = 16384


def draw_decay_log(key, part):
    pick_key, slow_key, fast_key = jax.random.split(jax.random.fold_in(key, 11), 3)
    slow_share = 0.5
    is_slow = jax.random.uniform(pick_key, (HEADS,), jnp.float32) < slow_share
    slow_rate = jax.random.uniform(slow_key, (HEADS,), jnp.float32, 0.25, 0.5) / TOKENS
    fast_rate = jax.random.uniform(fast_key, (HEADS,), jnp.float32, 0.05, 0.1)
    return jnp.log(jnp.where(is_slow, slow_rate, fast_rate)).astype(jnp.float32)


def draw_decay_pre(key, part):
    level_key, noise_key = jax.random.split(jax.random.fold_in(key, 23), 2)
    levels = jax.random.uniform(level_key, (HEADS, TOKENS // TOK_DEV), jnp.float32, -1.5, 1.0)
    noise = jax.random.uniform(noise_key, (HEADS, TOKENS), jnp.float32, -0.99, 0.99)
    return (jnp.repeat(levels, TOK_DEV, axis=1) + noise).astype(jnp.float32)


def raised(array, key, source, target, blocks, factor):
    def block_of(position):
        return (jnp.arange(array.shape[position]) // (array.shape[position] // blocks)).reshape((-1,) + (1,) * (array.ndim - 1 - position))

    one_side = jax.random.permutation(key, blocks)[block_of(target)]
    other_side = (block_of(target) + blocks // 2) % blocks
    return jnp.where((block_of(source) == one_side) | (block_of(source) == other_side), factor * array, array)


def steps_of(stream_key, shape, cuts, least, high):
    factor_of, own = 1.0, jax.random.fold_in(stream_key, 6)
    for dim, shards_of in cuts:
        heights = jnp.exp(jax.random.uniform(jax.random.fold_in(own, dim), (shards_of,), jnp.float32, least / len(cuts), high / len(cuts)))
        factor_of = factor_of * jnp.repeat(heights, shape[dim] // shards_of).reshape([-1 if axis == dim else 1 for axis in range(len(shape))])
    return factor_of


def bell_draw(key, shape, width, most, cuts=(), dtype=jnp.bfloat16):
    level = steps_of(key, shape, cuts, -0.22, 0.18) if cuts else 1.0
    drawn = jax.random.normal(key, shape, jnp.float32) * width * level
    return jnp.minimum(jnp.maximum(drawn, -most), most).astype(dtype)


def noise_with(own_key, dims, scale, most, cuts, heavy, kind=jnp.bfloat16):
    entries = scale * jax.random.normal(own_key, dims, jnp.float32)
    if cuts:
        entries = entries * steps_of(own_key, dims, cuts, -0.22, 0.18)
    return jnp.clip(raised(entries, jax.random.fold_in(own_key, 3), *heavy), -most, most).astype(kind)


def setup_inputs(seed: int = 0) -> dict:
    arg_keys = jax.random.split(jax.random.key(seed), 9)
    return {
        "block_input": noise_with(arg_keys[0], (TOKENS, D), 1.0, 6.0, ((0, 8),), (0, 1, 8, 2.0)),
        "value_weight": bell_draw(arg_keys[1], (D, HEADS * HEAD), D ** -0.5, 0.09375, ((1, 4),)),
        "key_rows": bell_draw(arg_keys[2], (TOKENS, GROUPS * STATE), 0.125, 1.0, ((0, 8), (1, 4))),
        "query_rows": bell_draw(arg_keys[3], (TOKENS, GROUPS * STATE), 0.125, 1.0, ((0, 8), (1, 4))),
        "decay_pre": draw_decay_pre(jax.random.fold_in(arg_keys[8], 71), 0),
        "decay_log": draw_decay_log(jax.random.fold_in(arg_keys[8], 71), 0),
        "gate_rows": bell_draw(arg_keys[6], (TOKENS, HEADS * HEAD), 1.0, 6.0, ((0, 8), (1, 4))),
        "out_grad": bell_draw(arg_keys[7], (TOKENS, HEADS * HEAD), 1.0, 6.0, ((0, 8), (1, 4))),
    }


HIGH = lax.Precision.HIGHEST

def block_mixer(values, key_float, query_float, step_sizes, log_steps, start_state):
    length, head_count, head_width = values.shape
    groups = key_float.shape[1]
    group_ratio = head_count // groups
    blocks = length // BLK
    value_blocks = values.reshape(blocks, BLK, head_count, head_width)
    key_blocks = jnp.repeat(key_float.reshape(blocks, BLK, groups, -1), group_ratio, axis=2)
    query_blocks = jnp.repeat(query_float.reshape(blocks, BLK, groups, -1), group_ratio, axis=2)
    step_blocks = step_sizes.reshape(head_count, blocks, BLK).transpose(1, 0, 2)
    running = jnp.cumsum(log_steps.reshape(head_count, blocks, BLK).transpose(1, 0, 2), axis=-1)
    lower = jnp.tril(jnp.ones((BLK, BLK), bool))
    spread = jnp.where(lower, running[..., :, None] - running[..., None, :], 0.0)
    decay = jnp.where(lower, jnp.exp(spread), 0.0)
    scores = jnp.einsum('cqhn,ckhn->chqk', query_blocks, key_blocks, precision=HIGH)
    weights = scores * decay * step_blocks[:, :, None, :]
    inner = jnp.einsum('chqk,ckhp->cqhp', weights, value_blocks, precision=HIGH)
    to_end = jnp.exp(running[..., -1:] - running) * step_blocks
    block_states = jnp.einsum('cqhn,chq,cqhp->chpn', key_blocks, to_end, value_blocks, precision=HIGH)
    factors = jnp.exp(running[..., -1])

    def advance(state_now, item):
        contrib, factor = item
        return (factor[:, None, None] * state_now + contrib, state_now)
    end_state, before = lax.scan(advance, start_state, (block_states, factors))
    outer = jnp.einsum('cqhn,chpn,chq->cqhp', query_blocks, before, jnp.exp(running), precision=HIGH)
    return ((inner + outer).reshape(length, head_count, head_width), end_state)

def reference(block_input, value_weight, key_rows, query_rows, decay_pre, decay_log, gate_rows, out_grad):
    head_count = decay_log.shape[0]
    length = block_input.shape[0]
    groups = key_rows.shape[1] // STATE
    projected = jnp.dot(block_input, value_weight, preferred_element_type=jnp.float32).astype(jnp.bfloat16)
    pre_float = lax.optimization_barrier(projected).astype(jnp.float32)
    sig_pre = jax.nn.sigmoid(pre_float)
    values = (pre_float * sig_pre).reshape(length, head_count, HEAD)
    step_sizes = jax.nn.softplus(decay_pre)
    decay_rates = jnp.exp(decay_log)
    log_steps = -decay_rates[:, None] * step_sizes
    key_float = key_rows.astype(jnp.float32).reshape(length, groups, STATE)
    query_float = query_rows.astype(jnp.float32).reshape(length, groups, STATE)
    gate_float = gate_rows.astype(jnp.float32)
    sig_gate = jax.nn.sigmoid(gate_float)
    cot_float = out_grad.astype(jnp.float32)
    zero_state = jnp.zeros((head_count, HEAD, STATE), jnp.float32)

    def forward(vals, krows, qrows, sizes, logs):
        mixed, _ = block_mixer(vals, krows, qrows, sizes, logs, zero_state)
        return mixed
    mixed, pullback = jax.vjp(forward, values, key_float, query_float, step_sizes, log_steps)
    grad_mixed = (cot_float * gate_float * sig_gate).reshape(length, head_count, HEAD)
    value_back, key_back, query_back, size_back, log_back = pullback(grad_mixed)
    gate_grad = cot_float * mixed.reshape(length, head_count * HEAD) * sig_gate * (1.0 + gate_float * (1.0 - sig_gate))
    size_total = size_back - decay_rates[:, None] * log_back
    decay_grad = size_total * jax.nn.sigmoid(decay_pre)
    value_grad = (value_back.reshape(length, head_count * HEAD) * sig_pre * (1.0 + pre_float * (1.0 - sig_pre))).astype(jnp.bfloat16)
    weight_grad = lax.dot_general(block_input, value_grad, (((0,), (0,)), ((), ())), preferred_element_type=jnp.float32)
    row_norms = lax.optimization_barrier(jnp.sum(weight_grad * weight_grad, axis=1))
    return (key_back.reshape(length, groups * STATE), query_back.reshape(length, groups * STATE), decay_grad, gate_grad, weight_grad, row_norms)
```

```python
import functools

import jax
import jax.numpy as jnp
from jax import lax
from jax.experimental import pallas as pl
from jax.experimental.pallas import tpu as pltpu
from jax.sharding import PartitionSpec as P

HEAD = 64
STATE = 64
BLK = 128

HIGH = lax.Precision.HIGHEST
BF = jnp.bfloat16
F32 = jnp.float32


def dot(a, b, ca, cb):
    return lax.dot_general(a, b, (((ca,), (cb,)), ((), ())), preferred_element_type=F32)


def load_chunk(pre_ref, gate_ref, out_ref):
    pre = pre_ref[...].astype(F32)
    gate = gate_ref[...].astype(F32)
    cot = out_ref[...].astype(F32)
    sig_pre = jax.nn.sigmoid(pre)
    sig_gate = jax.nn.sigmoid(gate)
    return pre, sig_pre, pre * sig_pre, gate, sig_gate, cot, cot * gate * sig_gate


def scales(cols_ref, heads):
    run = cols_ref[:, 0:heads]
    step = cols_ref[:, heads:2 * heads]
    end = cols_ref[BLK - 1:BLK, 0:heads]
    before = cols_ref[0:1, 2 * heads:3 * heads]
    return run, jnp.exp(run), jnp.exp(end - run) * step, jnp.exp(end), jnp.exp(before)


def states_kernel(heads, ratio, pre_ref, gate_ref, out_ref, key_ref, query_ref, cols_ref,
                  before_ref, end_ref, start_ref):
    @pl.when(pl.program_id(0) == 0)
    def _():
        end_ref[...] = jnp.zeros_like(end_ref)
        start_ref[...] = jnp.zeros_like(start_ref)

    _, _, vals, _, _, _, grads = load_chunk(pre_ref, gate_ref, out_ref)
    _, from_start, to_end, factor, before = scales(cols_ref, heads)
    before_ref[...] = end_ref[...]
    for h in range(heads):
        g = h // ratio
        sl = slice(h * HEAD, (h + 1) * HEAD)
        gs = slice(g * STATE, (g + 1) * STATE)
        contrib = dot(key_ref[:, gs], (vals[:, sl] * to_end[:, h:h + 1]).astype(BF), 0, 0)
        back = dot(query_ref[:, gs], (grads[:, sl] * from_start[:, h:h + 1]).astype(BF), 0, 0)
        end_ref[:, sl] = end_ref[:, sl] * factor[:, h:h + 1] + contrib
        start_ref[:, sl] = start_ref[:, sl] + before[:, h:h + 1] * back


def grads_kernel(heads, ratio, pre_ref, gate_ref, out_ref, key_ref, query_ref, cols_ref,
                 rows_ref, before_ref, in_ref, end_ref, outgo_ref,
                 dkey_ref, dquery_ref, dgate_ref, dval_ref, rc_ref, next_ref, dstate_ref):
    @pl.when(pl.program_id(0) == 0)
    def _():
        next_ref[...] = end_ref[...]
        dstate_ref[...] = outgo_ref[...]

    pre, sig_pre, vals, gate, sig_gate, cot, grads = load_chunk(pre_ref, gate_ref, out_ref)
    run, from_start, to_end, factor, before = scales(cols_ref, heads)
    at_q = lax.broadcasted_iota(jnp.int32, (BLK, BLK), 0)
    at_k = lax.broadcasted_iota(jnp.int32, (BLK, BLK), 1)
    lower = at_q >= at_k
    val_slope = sig_pre * (1.0 + pre * (1.0 - sig_pre))
    gate_slope = cot * sig_gate * (1.0 + gate * (1.0 - sig_gate))
    for g in range(heads // ratio):
        gs = slice(g * STATE, (g + 1) * STATE)
        key = key_ref[:, gs]
        query = query_ref[:, gs]
        scores = dot(query, key, 1, 1)
        total = None
        dkey = None
        dquery = None
        for h in range(g * ratio, (g + 1) * ratio):
            sl = slice(h * HEAD, (h + 1) * HEAD)
            spread = run[:, h:h + 1] - rows_ref[h:h + 1, :]
            decay = jnp.exp(jnp.where(lower, spread, -1e30)) * rows_ref[heads + h:heads + h + 1, :]
            weights = (scores * decay).astype(BF)
            val, grad = vals[:, sl], grads[:, sl]
            val_b, grad_b = val.astype(BF), grad.astype(BF)
            pulled = dot(grad_b, val_b, 1, 1) * decay
            total = pulled if total is None else total + pulled
            state = before_ref[:, sl] + before[:, h:h + 1] * in_ref[:, sl]
            dstate = dstate_ref[:, sl]
            state_b, dstate_b = state.astype(BF), dstate.astype(BF)
            fs, te = from_start[:, h:h + 1], to_end[:, h:h + 1]
            mixed = dot(weights, val_b, 1, 0) + dot(query, state_b, 1, 0) * fs
            dval = dot(weights, grad_b, 0, 0) + dot(key, dstate_b, 1, 0) * te
            grad_fs = (grad * fs).astype(BF)
            dq = dot(grad_fs, state_b, 1, 1)
            dk = dot((val * te).astype(BF), dstate_b, 1, 1)
            dquery = dq if dquery is None else dquery + dq
            dkey = dk if dkey is None else dkey + dk
            dgate_ref[:, sl] = mixed * gate_slope[:, sl]
            dval_ref[:, sl] = (dval * val_slope[:, sl]).astype(BF)
            cross = jnp.sum(jnp.sum(next_ref[:, sl] * dstate, axis=1, keepdims=True), axis=0,
                            keepdims=True)
            rc_ref[:, h:h + 1] = jnp.sum(grad * mixed, axis=1, keepdims=True)
            rc_ref[:, heads + h:heads + h + 1] = jnp.sum(val * dval, axis=1, keepdims=True)
            rc_ref[:, 2 * heads + h:2 * heads + h + 1] = jnp.broadcast_to(cross, (BLK, 1))
            next_ref[:, sl] = state
            dstate_ref[:, sl] = dstate * factor[:, h:h + 1] + dot(query, grad_fs, 0, 0)
        total_b = total.astype(BF)
        dquery_ref[:, gs] = dquery + dot(total_b, key, 1, 0)
        dkey_ref[:, gs] = dkey + dot(total_b, query, 0, 0)


def shards(
    block_input, value_weight, key_rows, query_rows, decay_pre, decay_log, gate_rows, out_grad
):
    heads = decay_log.shape[0]
    tokens = block_input.shape[0]
    groups = key_rows.shape[1] // STATE
    ratio = heads // groups
    wide, narrow = heads * HEAD, groups * STATE
    blocks = tokens // BLK
    projected = jnp.dot(block_input, value_weight, preferred_element_type=F32).astype(BF)

    step_sizes = jax.nn.softplus(decay_pre)
    rates = jnp.exp(decay_log)
    logs = (-rates[:, None] * step_sizes).reshape(heads, blocks, BLK)
    upto = jnp.triu(jnp.ones((BLK, BLK), F32))
    running = jnp.einsum("hbs,st->hbt", logs, upto, precision=HIGH)
    ends = running[:, :, -1]
    earlier = jnp.triu(jnp.ones((blocks, blocks), F32), 1)
    prefix = jnp.einsum("hb,bc->hc", ends, earlier, precision=HIGH)
    log_total = jnp.sum(ends, axis=1)
    rows = jnp.concatenate([running.reshape(heads, tokens), step_sizes], axis=0)
    prefix_rows = jnp.broadcast_to(prefix[:, :, None], (heads, blocks, BLK)).reshape(heads, tokens)
    cols = jnp.concatenate([rows, prefix_rows], axis=0).T

    def spec(width, rev):
        if rev:
            return pl.BlockSpec((BLK, width), lambda i: (blocks - 1 - i, 0))
        return pl.BlockSpec((BLK, width), lambda i: (i, 0))

    whole = pl.BlockSpec((STATE, wide), lambda i: (0, 0))
    state_shape = jax.ShapeDtypeStruct((STATE, wide), F32)
    params = pltpu.CompilerParams(dimension_semantics=("arbitrary",))
    before, end_state, start_grad = pl.pallas_call(
        functools.partial(states_kernel, heads, ratio),
        grid=(blocks,),
        in_specs=[spec(wide, False)] * 3 + [spec(narrow, False)] * 2 + [spec(3 * heads, False)],
        out_specs=[pl.BlockSpec((STATE, wide), lambda i: (i, 0)), whole, whole],
        out_shape=[jax.ShapeDtypeStruct((blocks * STATE, wide), F32), state_shape, state_shape],
        compiler_params=params,
        name="span_states",
    )(projected, gate_rows, out_grad, key_rows, query_rows, cols)

    lanes_total = jnp.repeat(log_total, HEAD)[None, :]
    packed = jnp.concatenate(
        [end_state, start_grad, jnp.broadcast_to(lanes_total, (8, wide))], axis=0
    )
    every = lax.all_gather(packed, "sp")
    count, index = lax.axis_size("sp"), lax.axis_index("sp")
    totals = every[:, 2 * STATE, :]
    s = jnp.arange(count)[:, None]
    j = jnp.arange(count)[None, :]
    ahead = jnp.sum(jnp.where(((s < j) & (j < index))[:, :, None], totals[None], 0.0), axis=1)
    after = jnp.sum(jnp.where(((s > j) & (j > index))[:, :, None], totals[None], 0.0), axis=1)
    ahead = jnp.where(s < index, jnp.exp(ahead), 0.0)
    after = jnp.where(s > index, jnp.exp(after), 0.0)
    incoming = jnp.sum(ahead[:, None, :] * every[:, :STATE], axis=0)
    outgoing = jnp.sum(after[:, None, :] * every[:, STATE:2 * STATE], axis=0)
    end_state = end_state + jnp.exp(lanes_total) * incoming

    key_grad, query_grad, gate_grad, value_grad, sums = pl.pallas_call(
        functools.partial(grads_kernel, heads, ratio),
        grid=(blocks,),
        in_specs=[spec(wide, True)] * 3 + [spec(narrow, True)] * 2 + [
            spec(3 * heads, True),
            pl.BlockSpec((2 * heads, BLK), lambda i: (0, blocks - 1 - i)),
            pl.BlockSpec((STATE, wide), lambda i: (blocks - 1 - i, 0)),
            whole, whole, whole,
        ],
        out_specs=[spec(narrow, True), spec(narrow, True), spec(wide, True), spec(wide, True),
                   spec(3 * heads, True)],
        out_shape=[
            jax.ShapeDtypeStruct((tokens, narrow), F32),
            jax.ShapeDtypeStruct((tokens, narrow), F32),
            jax.ShapeDtypeStruct((tokens, wide), F32),
            jax.ShapeDtypeStruct((tokens, wide), BF),
            jax.ShapeDtypeStruct((tokens, 3 * heads), F32),
        ],
        scratch_shapes=[pltpu.VMEM((STATE, wide), F32), pltpu.VMEM((STATE, wide), F32)],
        compiler_params=params,
        name="span_grads",
    )(projected, gate_rows, out_grad, key_rows, query_rows, cols, rows, before, incoming,
      end_state, outgoing)

    weight_grad = lax.psum_scatter(
        dot(block_input, value_grad, 0, 0), "sp", scatter_dimension=0, tiled=True
    )
    row_norms = lax.psum(jnp.sum(weight_grad * weight_grad, axis=1), "tp")

    sums = sums.T.reshape(3, heads, blocks, BLK)
    onward = jnp.einsum("hbs,ts->hbt", sums[0] - sums[1], upto, precision=HIGH)
    log_back = (onward + sums[2]).reshape(heads, tokens)
    size_total = sums[1].reshape(heads, tokens) / step_sizes - rates[:, None] * log_back
    decay_grad = size_total * jax.nn.sigmoid(decay_pre)
    return (key_grad, query_grad, decay_grad, gate_grad, weight_grad, row_norms)


def solution(mesh):
    in_specs = (
        P("sp", None),
        P(None, "tp"),
        P("sp", "tp"),
        P("sp", "tp"),
        P("tp", "sp"),
        P("tp"),
        P("sp", "tp"),
        P("sp", "tp"),
    )
    out_specs = (P("sp", "tp"), P("sp", "tp"), P("tp", "sp"), P("sp", "tp"), P("sp", "tp"), P("sp"))
    return jax.shard_map(shards, mesh=mesh, in_specs=in_specs, out_specs=out_specs, check_vma=False)
```
